32 devices in a mesh: sp: 8 (over z, x), tp: 4 (over y, core).
Axes of the slice: x: 2, y: 2, z: 4, core: 2. Of those that a mesh axis runs over, the one named last changes fastest.
Arguments:
- inputs: bfloat16 [4096, 4096], P('sp', 'tp'), may hold values from -6 to 6
- w_value: bfloat16 [4096, 4096], P(None, 'tp'), may hold values from -0.09375 to 0.09375
- w_gate: bfloat16 [4096, 4096], P(None, 'tp'), may hold values from -0.09375 to 0.09375
- taps: bfloat16 [31, 4096], P(None, 'tp'), may hold values from -1 to 1
- ln_gain: float32 [4096], P('tp'), may hold values from 0.1 to 1.9
- w_out: bfloat16 [4096, 4096], P(None, 'tp'), may hold values from -0.09375 to 0.09375
- grad_out: bfloat16 [4096, 4096], P('sp', 'tp'), may hold values from -6 to 6
Outputs:
- grad_input: bfloat16 [4096, 4096], P('sp', 'tp')
- grad_value_w: float32 [4096, 4096], P('sp', 'tp')
- grad_gate_w: float32 [4096, 4096], P('sp', 'tp')
- grad_out_w: float32 [4096, 4096], P('sp', 'tp')
- grad_taps: float32 [31, 4096], P(None, 'tp')
- grad_gain: float32 [4096], P('tp')
The draws below stay inside these ranges and needn't reach their ends.
All inputs are finite; a program needn't handle non-finite values.
Results may differ from the reference program's by a relative error of at most 0.017.
Values may be sent and summed in bfloat16 or wider, within the bound.
A program may use at most 128 MiB of HBM per device.

```python
import jax
import jax.numpy as jnp
from jax import lax

D = 4096
CONV = 31
SEQ = 4096
N_TP = 4


def with_spikes(result, key, source, target, shards_of, factor):
    def block_of(position):
        return (jnp.arange(result.shape[position]) // (result.shape[position] // shards_of)).reshape((-1,) + (1,) * (result.ndim - 1 - position))

    first = jax.random.permutation(key, shards_of)[block_of(target)]
    second = (block_of(target) + shards_of // 2) % shards_of
    return jnp.where((block_of(source) == first) | (block_of(source) == second), factor * result, result)


def block_scale(key, dims, cuts, low, high):
    def one(axis_at, shards_of):
        draws = jax.random.uniform(jax.random.fold_in(jax.random.fold_in(key, 6), axis_at), (shards_of,), jnp.float32, low / len(cuts), high / len(cuts))
        return jnp.repeat(jnp.exp(draws), dims[axis_at] // shards_of).reshape((-1,) + (1,) * (len(dims) - axis_at - 1))

    gain = one(*cuts[0])
    for cut in cuts[1:]:
        gain = gain * one(*cut)
    return gain


def noise(rng, shape, spread, limit, split=(), held_as=jnp.bfloat16):
    array = spread * jax.random.normal(rng, shape, jnp.float32)
    if split:
        array = array * block_scale(rng, shape, split, -0.22, 0.18)
    return jnp.clip(array, -limit, limit).astype(held_as)


def heavy_noise(own_key, extent, spread, bound, split, heavy, kind=jnp.bfloat16):
    drawn = spread * jax.random.normal(own_key, extent, jnp.float32)
    if split:
        drawn = drawn * block_scale(own_key, extent, split, -0.22, 0.18)
    return jnp.clip(with_spikes(drawn, jax.random.fold_in(own_key, 3), *heavy), -bound, bound).astype(kind)


def setup_inputs(seed: int = 0) -> dict:
    arg_keys = jax.random.split(jax.random.key(seed), 8)
    return {
        "inputs": heavy_noise(arg_keys[0], (SEQ, D), 1.0, 6.0, ((0, 8), (1, 4)), (0, 1, 8, 2.0)),
        "w_value": noise(arg_keys[1], (D, D), D ** -0.5, 0.09375, ((1, 4),)),
        "w_gate": noise(arg_keys[2], (D, D), D ** -0.5, 0.09375, ((1, 4),)),
        "taps": noise(arg_keys[3], (CONV, D), CONV ** -0.5, 1.0, ((1, 4),)),
        "ln_gain": jnp.clip(1.0 + 0.18 * jax.random.normal(arg_keys[4], (D,), jnp.float32), 0.1, 1.9),
        "w_out": noise(arg_keys[5], (D, D), D ** -0.5, 0.09375, ((1, 4),)),
        "grad_out": heavy_noise(arg_keys[6], (SEQ, D), 1.0, 6.0, ((0, 8), (1, 4)), (0, 1, 8, 2.0)),
    }


def contract_tokens(left, right):
    return lax.dot_general(left, right, (((0,), (0,)), ((), ())), preferred_element_type=jnp.float32)

def contract_channels(left, right):
    return lax.dot_general(left, right, (((1,), (1,)), ((), ())), preferred_element_type=jnp.float32)

def reference(inputs, w_value, w_gate, taps, ln_gain, w_out, grad_out):
    seq_len = inputs.shape[0]
    full_width = inputs.shape[1]
    radius = taps.shape[0] // 2
    pre_value = jnp.dot(inputs, w_value, preferred_element_type=jnp.float32)
    pre_gate = jnp.dot(inputs, w_gate, preferred_element_type=jnp.float32)
    gate_sigmoid = jax.nn.sigmoid(pre_gate)
    hidden = (pre_value * gate_sigmoid).astype(jnp.bfloat16)
    padded = jnp.pad(hidden.astype(jnp.float32), ((radius, radius), (0, 0)))
    tap_values = taps.astype(jnp.float32)
    convolved = jnp.zeros((seq_len, full_width), jnp.float32)
    for offset in range(taps.shape[0]):
        convolved = convolved + tap_values[offset] * padded[offset:offset + seq_len]
    mean = lax.optimization_barrier(jnp.sum(convolved, axis=1, keepdims=True)) / full_width
    variance = lax.optimization_barrier(jnp.sum(convolved * convolved, axis=1, keepdims=True)) / full_width - mean * mean
    inverse = lax.rsqrt(variance + 1e-06)
    normed = (convolved - mean) * inverse
    scaled = normed * ln_gain
    activated = jax.nn.silu(scaled).astype(jnp.bfloat16)
    grad_act = jnp.dot(grad_out, w_out, preferred_element_type=jnp.float32)
    sig_scaled = jax.nn.sigmoid(scaled)
    grad_scaled = grad_act * sig_scaled * (1.0 + scaled * (1.0 - sig_scaled))
    grad_gain = lax.optimization_barrier(jnp.sum(grad_scaled * normed, axis=0))
    grad_normed = grad_scaled * ln_gain
    first_sum = lax.optimization_barrier(jnp.sum(grad_normed, axis=1, keepdims=True)) / full_width
    second_sum = lax.optimization_barrier(jnp.sum(grad_normed * normed, axis=1, keepdims=True)) / full_width
    grad_conv = inverse * (grad_normed - first_sum - normed * second_sum)
    tap_rows = []
    for offset in range(taps.shape[0]):
        tap_rows.append(lax.optimization_barrier(jnp.sum(padded[offset:offset + seq_len] * grad_conv, axis=0)))
    grad_taps = jnp.stack(tap_rows, axis=0)
    grad_padded = jnp.pad(grad_conv, ((radius, radius), (0, 0)))
    grad_hidden = jnp.zeros((seq_len, full_width), jnp.float32)
    for offset in range(taps.shape[0]):
        begin = 2 * radius - offset
        grad_hidden = grad_hidden + tap_values[offset] * grad_padded[begin:begin + seq_len]
    grad_value = (grad_hidden * gate_sigmoid).astype(jnp.bfloat16)
    grad_gate = (grad_hidden * pre_value * gate_sigmoid * (1.0 - gate_sigmoid)).astype(jnp.bfloat16)
    grad_value_w = contract_tokens(inputs, grad_value)
    grad_gate_w = contract_tokens(inputs, grad_gate)
    grad_out_w = contract_tokens(grad_out, activated)
    block = full_width // N_TP
    total = jnp.zeros((seq_len, full_width), jnp.float32)
    for index in range(N_TP):
        lower = index * block
        partial_value = contract_channels(grad_value[:, lower:lower + block], w_value[:, lower:lower + block])
        partial_value = partial_value + contract_channels(grad_gate[:, lower:lower + block], w_gate[:, lower:lower + block])
        rounded = lax.optimization_barrier(partial_value.astype(jnp.bfloat16))
        total = total + rounded.astype(jnp.float32)
    grad_input = total.astype(jnp.bfloat16)
    return (grad_input, grad_value_w, grad_gate_w, grad_out_w, grad_taps, grad_gain)
```

```python
import jax
import jax.numpy as jnp
from jax import lax
from jax.sharding import Mesh, PartitionSpec as P


SP = ("outer", "pair")


def shifted(value, steps):
    count = lax.axis_size(SP)
    leading, last = (max(0, -steps), min(count, count - steps))
    return lax.ppermute(value, SP, [(source, source + steps) for source in range(leading, last)])


def with_halo(cells, width):
    head, tail = cells[:width], cells[cells.shape[0] - width :]
    return jnp.concatenate([shifted(tail, 1), cells, shifted(head, -1)], axis=0)


def swap(value):
    return lax.ppermute(value, "pair", [(0, 1), (1, 0)])


def sum_tokens(value):
    count, step = lax.axis_size(SP), 1
    while step < count:
        value = value + lax.ppermute(value, SP, [(i, i ^ step) for i in range(count)])
        step *= 2
    return value


def parity_columns(value, block, parity):
    rows, width = value.shape
    split = value.reshape(rows, width // (2 * block), 2, block)
    return lax.dynamic_index_in_dim(split, parity, 2, keepdims=False).reshape(rows, width // 2)


def contract_tokens(left, right):
    return lax.dot_general(
        left, right, (((0,), (0,)), ((), ())), preferred_element_type=jnp.float32
    )


def contract_channels(left, right):
    return lax.dot_general(
        left, right, (((1,), (1,)), ((), ())), preferred_element_type=jnp.float32
    )


def scatter_rows(value):
    return lax.psum_scatter(
        value.astype(jnp.bfloat16), "outer", scatter_dimension=0, tiled=True
    ).astype(jnp.float32)


def scatter_channels(value):
    count, me = lax.axis_size("tp"), lax.axis_index("tp")
    width = value.shape[1] // count

    def part(owner):
        return lax.dynamic_slice_in_dim(value, lax.rem(owner, count) * width, width, axis=1)

    total = part(me).astype(jnp.float32)
    for step in range(1, count):
        sent = lax.ppermute(part(me + step), "tp", [(i, (i + step) % count) for i in range(count)])
        total = total + sent.astype(jnp.float32)
    return total.astype(jnp.bfloat16)


def local(inputs, w_value, w_gate, taps, ln_gain, w_out, grad_out):
    tok_rows = inputs.shape[0]
    own_width = w_value.shape[1]
    full_width = inputs.shape[1] * lax.axis_size("tp")
    radius = taps.shape[0] // 2
    full_inputs, full_grads = (
        lax.all_gather(inputs, "tp", axis=1, tiled=True),
        lax.all_gather(grad_out, "tp", axis=1, tiled=True),
    )
    own = lax.axis_index("pair")
    block = full_width // lax.axis_size(SP)
    crossing = jnp.concatenate([parity_columns(cells, block, 1 - own) for cells in (grad_out, inputs)], axis=0)
    crossed = lax.all_gather(swap(crossing), "tp", axis=1, tiled=True)
    pair_grads = jnp.concatenate([parity_columns(full_grads, block, own), crossed[:tok_rows]], axis=0)
    own_columns, pair_columns = parity_columns(full_inputs, block, own), crossed[tok_rows:]
    pre_value = jnp.dot(full_inputs, w_value, preferred_element_type=jnp.float32)
    pre_gate = jnp.dot(full_inputs, w_gate, preferred_element_type=jnp.float32)
    gate_sigmoid = jax.nn.sigmoid(pre_gate)
    hidden = (pre_value * gate_sigmoid).astype(jnp.bfloat16)
    padded = with_halo(hidden, radius).astype(jnp.float32)
    tap_values = taps.astype(jnp.float32)
    convolved = jnp.zeros((tok_rows, own_width), jnp.float32)
    for offset in range(taps.shape[0]):
        convolved = convolved + tap_values[offset] * padded[offset : offset + tok_rows]
    sum_first, sum_square = lax.psum(
        (jnp.sum(convolved, axis=1), jnp.sum(convolved * convolved, axis=1)), "tp"
    )
    mean = (sum_first / full_width)[:, None]
    variance = (sum_square / full_width)[:, None] - mean * mean
    inverse = lax.rsqrt(variance + 1e-06)
    normed = (convolved - mean) * inverse
    scaled = normed * ln_gain
    activated = jax.nn.silu(scaled).astype(jnp.bfloat16)
    pair_activated = jnp.concatenate([activated, swap(activated)], axis=0)
    grad_act = jnp.dot(full_grads, w_out, preferred_element_type=jnp.float32)
    sig_scaled = jax.nn.sigmoid(scaled)
    grad_scaled = grad_act * sig_scaled * (1.0 + scaled * (1.0 - sig_scaled))
    gain_part = jnp.sum(grad_scaled * normed, axis=0)
    grad_normed = grad_scaled * ln_gain
    first_sum, second_sum = lax.psum(
        (jnp.sum(grad_normed, axis=1), jnp.sum(grad_normed * normed, axis=1)), "tp"
    )
    grad_conv = inverse * (
        grad_normed
        - (first_sum / full_width)[:, None]
        - normed * (second_sum / full_width)[:, None]
    )
    tap_rows = []
    for offset in range(taps.shape[0]):
        tap_rows.append(jnp.sum(padded[offset : offset + tok_rows] * grad_conv, axis=0))
    token_sums = sum_tokens(jnp.stack(tap_rows + [gain_part], axis=0))
    grad_taps, grad_gain = token_sums[:-1], token_sums[-1]
    spread = jnp.zeros((tok_rows + 2 * radius, own_width), jnp.float32)
    for offset in range(taps.shape[0]):
        spread = spread + tap_values[offset] * jnp.pad(
            grad_conv, ((offset, 2 * radius - offset), (0, 0))
        )
    from_before = shifted(spread[tok_rows + radius :], 1)
    from_after = shifted(spread[:radius], -1)
    grad_hidden = spread[radius : radius + tok_rows]
    grad_hidden = grad_hidden + jnp.pad(from_before, ((0, tok_rows - radius), (0, 0)))
    grad_hidden = grad_hidden + jnp.pad(from_after, ((tok_rows - radius, 0), (0, 0)))
    grad_value = (grad_hidden * gate_sigmoid).astype(jnp.bfloat16)
    grad_gate = (grad_hidden * pre_value * gate_sigmoid * (1.0 - gate_sigmoid)).astype(jnp.bfloat16)
    partial_value = contract_channels(grad_value, w_value) + contract_channels(grad_gate, w_gate)
    grad_input = scatter_channels(partial_value.astype(jnp.bfloat16))
    value_sum = contract_tokens(own_columns, grad_value) + contract_tokens(
        pair_columns, swap(grad_value)
    )
    gate_sum = contract_tokens(own_columns, grad_gate) + contract_tokens(
        pair_columns, swap(grad_gate)
    )
    grad_out_w = scatter_rows(contract_tokens(pair_grads, pair_activated))
    grad_value_w = scatter_rows(value_sum)
    grad_gate_w = scatter_rows(gate_sum)
    return (grad_input, grad_value_w, grad_gate_w, grad_out_w, grad_taps, grad_gain)


def solution(mesh):
    count, across = mesh.devices.shape
    fine = Mesh(mesh.devices.reshape(count // 2, 2, across), ("outer", "pair", "tp"))
    in_specs = (
        P(SP, "tp"),
        P(None, "tp"),
        P(None, "tp"),
        P(None, "tp"),
        P("tp"),
        P(None, "tp"),
        P(SP, "tp"),
    )
    out_specs = (P(SP, "tp"), P(SP, "tp"), P(SP, "tp"), P(SP, "tp"), P(None, "tp"), P("tp"))
    return jax.shard_map(local, mesh=fine, in_specs=in_specs, out_specs=out_specs, check_vma=False)
```
